32 devices in a mesh: gr: 2 (over y), sp: 4 (over z), tp: 4 (over x, core).
Axes of the slice: x: 2, y: 2, z: 4, core: 2. Of those that a mesh axis runs over, the one named last changes fastest.
Arguments:
- tokens: bfloat16 [4, 1024, 4096], P('gr', ('sp', 'tp')), parts along dimension 0, may hold values from -6 to 6
- norm_gain: bfloat16 [4096], replicated, may hold values from 0.099609375 to 1.8984375
- key_weight: bfloat16 [4096, 1024], P(None, 'tp'), may hold values from -0.09375 to 0.09375
- value_weight: bfloat16 [4096, 1024], P(None, 'tp'), may hold values from -0.09375 to 0.09375
- cum_gates: float32 [4, 1024, 16], P('gr', 'sp', 'tp'), parts along dimension 0, may hold values from -173 to 0, as said below
- new_query: bfloat16 [4, 1024], P('gr', 'tp'), parts along dimension 0, may hold values from -240 to 240
- new_key: bfloat16 [4, 1024], P('gr', 'tp'), parts along dimension 0, may hold values from -6 to 6
- new_value: bfloat16 [4, 1024], P('gr', 'tp'), parts along dimension 0, may hold values from -6 to 6
- new_gate: float32 [4, 16], P('gr', 'tp'), parts along dimension 0, may hold values from -5 to -1.5
Outputs:
- key_cache: bfloat16 [4, 1024, 1024], P('gr', 'sp', 'tp'), parts along dimension 0
- value_cache: bfloat16 [4, 1024, 1024], P('gr', 'sp', 'tp'), parts along dimension 0
- readout: bfloat16 [4, 1024], P('gr', 'tp'), parts along dimension 0
The draws below stay inside these ranges and needn't reach their ends.
There are 2 independent parts, one for each index of `gr`. The reference program is written for one: setup_inputs(seed, part) draws one part's arguments, and reference() takes and returns one part's arrays. A program takes and returns all parts, laid end to end along the dimension named above; an argument that names none is the same for every part. Nothing has to cross between parts.
Inputs may be any that keep to these rules, and one draw needn't show every extreme that they name: `cum_gates`: along positions, for each prompt and head, the values never rise.
All inputs are finite; a program needn't handle non-finite values.
Results may differ from the reference program's by a relative error of at most 0.005.
The reference program's roundings to bfloat16 on the way (of `normed`) count: a program that leaves them out, or rounds other values in their place, can miss the bound.
Values may be sent and summed in bfloat16 or wider, within the bound.
A program may use at most 64 MiB of HBM per device.

```python
import jax
import jax.numpy as jnp
from jax import lax

D = 4096
HEAD_COUNT = 16
HD = 64
PROMPTS_PER_GROUP = 2
KW = 1024
PROMPT_LENGTH = 1024


def draw_cum_gates(key, part):
    key_pieces = jax.random.split(jax.random.fold_in(key, 11), 7)
    decaying_heads = jax.random.uniform(key_pieces[0], (PROMPTS_PER_GROUP, 1, HEAD_COUNT)) < 0.5
    slow_rate = jax.random.uniform(key_pieces[1], (PROMPTS_PER_GROUP, 1, HEAD_COUNT), jnp.float32, 0.5, 1.5) / PROMPT_LENGTH
    fast_rate = 1.0 / jax.random.uniform(key_pieces[2], (PROMPTS_PER_GROUP, 1, HEAD_COUNT), jnp.float32, 30.0, 100.0)
    base_rate = jnp.where(decaying_heads, slow_rate, fast_rate)
    block_size = max(PROMPT_LENGTH // 32, 1)
    token_positions = jnp.arange(PROMPT_LENGTH)
    block_ids = jnp.minimum(token_positions // block_size, 31)
    log_factor = jax.random.uniform(key_pieces[3], (PROMPTS_PER_GROUP, 32, HEAD_COUNT), jnp.float32, -1.05, 1.05)
    block_factor = jnp.exp(log_factor)[:, block_ids, :]
    noise = jax.random.uniform(key_pieces[4], (PROMPTS_PER_GROUP, PROMPT_LENGTH, HEAD_COUNT), jnp.float32, 0.5, 1.5)
    per_step_decay = base_rate * block_factor * noise
    segment_position = jax.random.randint(key_pieces[5], (PROMPTS_PER_GROUP, 3, HEAD_COUNT), 0, PROMPT_LENGTH)
    segment_length = jax.random.uniform(key_pieces[6], (PROMPTS_PER_GROUP, 3, HEAD_COUNT), jnp.float32, 0.22, 0.69)
    match_count = (token_positions[None, :, None, None] == segment_position[:, None, :, :]).astype(jnp.float32)
    prompt_segments = jnp.sum(match_count * segment_length[:, None, :, :], axis=2)
    per_step_decay = per_step_decay + prompt_segments * decaying_heads.astype(jnp.float32)
    return -jnp.cumsum(per_step_decay, axis=1)


def draw_new_query(key, part):
    key_pieces = jax.random.split(jax.random.fold_in(key, 23), 1)
    normal_part = jax.random.normal(key_pieces[0], (PROMPTS_PER_GROUP, HEAD_COUNT, HD), jnp.float32)
    values_out = jnp.clip(normal_part * 2.0, -12.0, 12.0)
    return values_out.reshape(PROMPTS_PER_GROUP, KW).astype(jnp.bfloat16)


def levels(key, shape, shards, least, largest):
    level, own = 1.0, jax.random.fold_in(key, 6)
    for dim, shards_of in shards:
        draws = jnp.exp(jax.random.uniform(jax.random.fold_in(own, dim), (shards_of,), jnp.float32, least / len(shards), largest / len(shards)))
        level = level * jnp.repeat(draws, shape[dim] // shards_of).reshape([-1 if axis == dim else 1 for axis in range(len(shape))])
    return level


def bell_draw(rng, shape, scale, most, cuts=(), kind=jnp.bfloat16):
    factor_of = levels(rng, shape, cuts, -0.22, 0.18) if cuts else 1.0
    result = jax.random.normal(rng, shape, jnp.float32) * scale * factor_of
    return jnp.minimum(jnp.maximum(result, -most), most).astype(kind)


def setup_inputs(seed: int = 0, part: int = 0) -> dict:
    key_list = jax.random.split(jax.random.key(seed), 10)
    part_keys = jax.random.split(jax.random.fold_in(key_list[9], part), 10)
    return {
        "tokens": bell_draw(part_keys[0], (PROMPTS_PER_GROUP, PROMPT_LENGTH, D), 1.0, 6.0, ((1, 16),)),
        "norm_gain": jnp.clip(1.0 + 0.18 * jax.random.normal(key_list[1], (D,), jnp.float32), 0.099609375, 1.8984375).astype(jnp.bfloat16),
        "key_weight": bell_draw(key_list[2], (D, KW), D ** -0.5, 0.09375, ((1, 4),)),
        "value_weight": bell_draw(key_list[3], (D, KW), D ** -0.5, 0.09375, ((1, 4),)),
        "cum_gates": draw_cum_gates(jax.random.fold_in(jax.random.fold_in(key_list[9], part), 71), part),
        "new_query": draw_new_query(jax.random.fold_in(jax.random.fold_in(key_list[9], part), 71), part),
        "new_key": bell_draw(part_keys[6], (PROMPTS_PER_GROUP, KW), 1.0, 6.0, ((1, 4),)),
        "new_value": bell_draw(part_keys[7], (PROMPTS_PER_GROUP, KW), 1.0, 6.0, ((1, 4),)),
        "new_gate": jnp.clip(-5.0 + 3.5 * jax.random.uniform(part_keys[8], (PROMPTS_PER_GROUP, HEAD_COUNT), jnp.float32) ** levels(part_keys[8], (PROMPTS_PER_GROUP, HEAD_COUNT), ((1, 4),), -0.2, 0.2), -5.0, -1.5),
    }


epsilon = 1e-06

def reference(tokens, norm_gain, key_weight, value_weight, cum_gates, new_query, new_key, new_value, new_gate):
    as_float = tokens.astype(jnp.float32)
    normed = (as_float * lax.rsqrt(lax.optimization_barrier(jnp.mean(as_float * as_float, axis=-1, keepdims=True)) + epsilon) * norm_gain.astype(jnp.float32)).astype(jnp.bfloat16)
    flat_rows = normed.reshape(PROMPTS_PER_GROUP * PROMPT_LENGTH, D)
    key_cache = jnp.dot(flat_rows, key_weight, preferred_element_type=jnp.float32).astype(jnp.bfloat16).reshape(PROMPTS_PER_GROUP, PROMPT_LENGTH, KW)
    value_cache = jnp.dot(flat_rows, value_weight, preferred_element_type=jnp.float32).astype(jnp.bfloat16).reshape(PROMPTS_PER_GROUP, PROMPT_LENGTH, KW)
    score_scale = HD ** (-0.5)
    queries = new_query.reshape(PROMPTS_PER_GROUP, HEAD_COUNT, HD).astype(jnp.float32)
    key_heads = key_cache.reshape(PROMPTS_PER_GROUP, PROMPT_LENGTH, HEAD_COUNT, HD).astype(jnp.float32)
    value_heads = value_cache.reshape(PROMPTS_PER_GROUP, PROMPT_LENGTH, HEAD_COUNT, HD).astype(jnp.float32)
    fresh_key = new_key.reshape(PROMPTS_PER_GROUP, HEAD_COUNT, HD).astype(jnp.float32)
    fresh_value = new_value.reshape(PROMPTS_PER_GROUP, HEAD_COUNT, HD).astype(jnp.float32)
    scores = jnp.einsum('shd,slhd->shl', queries, key_heads, precision=lax.Precision.HIGHEST) * score_scale
    scores = scores + (new_gate + cum_gates[:, PROMPT_LENGTH - 1, :])[:, :, None] - jnp.transpose(cum_gates, (0, 2, 1))
    fresh_score = lax.optimization_barrier(jnp.sum(queries * fresh_key, axis=-1)) * score_scale
    maxima = jnp.maximum(lax.optimization_barrier(jnp.max(scores, axis=-1)), fresh_score)
    weights = jnp.exp(scores - maxima[:, :, None])
    fresh_weight = jnp.exp(fresh_score - maxima)
    totals = lax.optimization_barrier(jnp.sum(weights, axis=-1)) + fresh_weight
    weighted = jnp.einsum('shl,slhd->shd', weights, value_heads, precision=lax.Precision.HIGHEST)
    weighted = weighted + fresh_weight[:, :, None] * fresh_value
    readout = (weighted / totals[:, :, None]).reshape(PROMPTS_PER_GROUP, KW).astype(jnp.bfloat16)
    return (key_cache, value_cache, readout)
```

```python
import functools

import jax
import jax.numpy as jnp
from jax import lax
from jax.experimental import pallas as pl
from jax.experimental.pallas import tpu as pltpu
from jax.sharding import PartitionSpec as P

HD = 64
CORES = 2

epsilon = 1e-06
masked_score = -1e30
MESH = pl.DeviceIdType.MESH


def kernel(
    dims,
    tok_hbm, gain_hbm, wk_hbm, wv_hbm, gates_hbm, q_hbm, nk_hbm, nv_hbm, ng_hbm,
    kc_hbm, vc_hbm, ro_ref,
    raw, nbuf, wbuf, kbuf, vbuf, gain_v, gates_v, q_v, nk_v, nv_v, ng_v, stats,
    loc_sem, w_sem, small_sem, out_sem,
    sx_sem, rx_sem, sp_sem, rp_sem, sr_sem, rr_sem, sz_sem, rz_sem,
):
    S, L, R, T, Z = dims
    X = T // CORES
    per = L // R
    NC = S * per
    C = kbuf.shape[2]
    H = C // HD
    BL = T * L
    tp = lax.axis_index("tp")
    z = lax.axis_index("sp")
    x, c = tp // CORES, tp % CORES
    partner = x * CORES + (CORES - 1 - c)

    def rows(j):
        return pl.ds(pl.multiple_of(j * R, R), R)

    for j in range(NC):
        pltpu.make_async_copy(tok_hbm.at[rows(j)], raw.at[tp, rows(j)], loc_sem.at[j]).start()
    w_copies = [
        pltpu.make_async_copy(wk_hbm, wbuf.at[:, pl.ds(0, C)], w_sem.at[0]),
        pltpu.make_async_copy(wv_hbm, wbuf.at[:, pl.ds(C, C)], w_sem.at[1]),
    ]
    small = [
        pltpu.make_async_copy(src, dst, small_sem.at[i])
        for i, (src, dst) in enumerate(
            [(gain_hbm, gain_v), (gates_hbm, gates_v), (q_hbm, q_v), (nk_hbm, nk_v), (nv_hbm, nv_v), (ng_hbm, ng_v)]
        )
    ]
    for copy in small + w_copies:
        copy.start()

    barrier = pltpu.get_barrier_semaphore()
    pl.semaphore_signal(barrier, inc=1, device_id={"tp": partner}, device_id_type=MESH)
    for d in range(1, X):
        pl.semaphore_signal(
            barrier, inc=1, device_id={"tp": ((x + d) % X) * CORES + c}, device_id_type=MESH
        )
    for d in range(1, Z):
        pl.semaphore_signal(barrier, inc=1, device_id={"sp": (z + d) % Z}, device_id_type=MESH)
    pl.semaphore_wait(barrier, 1 + (X - 1) + (Z - 1))

    def x_copy(d, j):
        return pltpu.make_async_remote_copy(
            raw.at[tp, rows(j)], raw.at[tp, rows(j)], sx_sem.at[d - 1, j], rx_sem.at[d - 1, j],
            device_id={"tp": ((x + d) % X) * CORES + c}, device_id_type=MESH,
        )

    def x_source(d, core):
        return ((x + X - d) % X) * CORES + core

    def relay_copy(d, j):
        t = x_source(d, c)
        return pltpu.make_async_remote_copy(
            raw.at[t, rows(j)], raw.at[t, rows(j)], sr_sem.at[d - 1, j], rr_sem.at[d - 1, j],
            device_id={"tp": partner}, device_id_type=MESH,
        )

    def arrival(t, j, sem):
        return pltpu.make_async_remote_copy(
            raw.at[t, rows(j)], raw.at[t, rows(j)], sem, sem,
            device_id={"tp": partner}, device_id_type=MESH,
        )

    for j in range(NC):
        pltpu.make_async_copy(tok_hbm.at[rows(j)], raw.at[tp, rows(j)], loc_sem.at[j]).wait()
        for d in range(1, X):
            x_copy(d, j).start()
    own_to_partner = pltpu.make_async_remote_copy(
        raw.at[tp], raw.at[tp], sp_sem, rp_sem, device_id={"tp": partner}, device_id_type=MESH
    )
    own_to_partner.start()

    for copy in small:
        copy.wait()
    gain = gain_v[...].astype(jnp.float32)

    def norm_into(t, j, at):
        v = raw[t, rows(j), :].astype(jnp.float32)
        r = lax.rsqrt(jnp.mean(v * v, axis=-1, keepdims=True) + epsilon)
        nbuf[pl.ds(pl.multiple_of(at, R), R), :] = (v * r * gain).astype(jnp.bfloat16)

    def project(count):
        return jnp.dot(
            nbuf[pl.ds(0, count), :], wbuf[...], preferred_element_type=jnp.float32
        ).astype(jnp.bfloat16)

    def keep(y, t, s, row, count):
        at = pl.ds(pl.multiple_of(t * L + row, R), count)
        kbuf[s, at, :] = y[:, :C]
        vbuf[s, at, :] = y[:, C:]

    def whole_source(t):
        def one(j, carry):
            norm_into(t, j, j * R)
            return carry

        lax.fori_loop(0, NC, one, 0)
        y = project(S * L)
        for s in range(S):
            keep(y[s * L : (s + 1) * L], t, s, 0, L)

    def near(i, carry):
        @pl.when(i == 1)
        def _():
            pltpu.make_async_remote_copy(
                raw.at[partner], raw.at[partner], sp_sem, rp_sem, device_id={"tp": partner}, device_id_type=MESH
            ).wait_recv()

        whole_source(x * CORES + (c + i) % CORES)
        return carry

    for copy in w_copies:
        copy.wait()
    lax.fori_loop(0, CORES, near, 0)

    def far(j, carry):
        for d in range(1, X):
            arrival(x_source(d, c), j, rx_sem.at[d - 1, j]).wait_recv()
            relay_copy(d, j).start()
        for d in range(1, X):
            norm_into(x_source(d, c), j, (d - 1) * R)
        for d in range(1, X):
            arrival(x_source(d, CORES - 1 - c), j, rr_sem.at[d - 1, j]).wait_recv()
            norm_into(x_source(d, CORES - 1 - c), j, (X - 1 + d - 1) * R)
        y = project(2 * (X - 1) * R)
        s, row = j // per, (j % per) * R
        for d in range(1, X):
            a, b = (d - 1) * R, (X - 1 + d - 1) * R
            keep(y[a : a + R], x_source(d, c), s, row, R)
            keep(y[b : b + R], x_source(d, CORES - 1 - c), s, row, R)
        return carry

    if X > 1:
        lax.fori_loop(0, NC, far, 0)

    outs = [
        pltpu.make_async_copy(kbuf, kc_hbm, out_sem.at[0]),
        pltpu.make_async_copy(vbuf, vc_hbm, out_sem.at[1]),
    ]
    for copy in outs:
        copy.start()

    scale = HD ** (-0.5)
    head_of_lane = lax.broadcasted_iota(jnp.int32, (H, C), 1) // HD
    own_head = head_of_lane == lax.broadcasted_iota(jnp.int32, (H, C), 0)
    eye = lax.broadcasted_iota(jnp.int32, (H, H), 0) == lax.broadcasted_iota(jnp.int32, (H, H), 1)
    last_block = z == Z - 1

    def as_row(column):
        return jnp.sum(jnp.where(own_head, column, 0.0), axis=0, keepdims=True)

    for s in range(S):
        qd = jnp.where(own_head, q_v[s : s + 1, :].astype(jnp.float32), 0.0)
        fresh = jnp.sum(qd * nk_v[s : s + 1, :].astype(jnp.float32), axis=1, keepdims=True) * scale
        gates = gates_v[s]
        own_gate = jnp.sum(jnp.where(eye, ng_v[s : s + 1, :], 0.0), axis=1, keepdims=True)
        fresh = jnp.where(last_block, fresh - (gates[:, BL - 1 : BL] + own_gate), masked_score)
        scores = lax.dot_general(
            qd.astype(jnp.bfloat16), kbuf[s], (((1,), (1,)), ((), ())), preferred_element_type=jnp.float32
        )
        scores = scores * scale - gates
        top = jnp.maximum(jnp.max(scores, axis=1, keepdims=True), fresh)
        weights = jnp.exp(scores - top)
        fresh_weight = jnp.exp(fresh - top)
        total = jnp.sum(weights, axis=1, keepdims=True) + fresh_weight
        high = weights.astype(jnp.bfloat16)
        low = (weights - high.astype(jnp.float32)).astype(jnp.bfloat16)
        values = vbuf[s]
        weighted = jnp.dot(high, values, preferred_element_type=jnp.float32)
        weighted = weighted + jnp.dot(low, values, preferred_element_type=jnp.float32)
        weighted = weighted + fresh_weight * nv_v[s : s + 1, :].astype(jnp.float32)
        stats[z, 0, s : s + 1, :] = as_row(top)
        stats[z, 1, s : s + 1, :] = as_row(total)
        stats[z, 2, s : s + 1, :] = as_row(weighted)

    def z_copy(d):
        return pltpu.make_async_remote_copy(
            stats.at[z], stats.at[z], sz_sem.at[d - 1], rz_sem.at[d - 1],
            device_id={"sp": (z + d) % Z}, device_id_type=MESH,
        )

    for d in range(1, Z):
        z_copy(d).start()
    for d in range(1, X):
        for j in range(NC):
            x_copy(d, j).wait_send()
            relay_copy(d, j).wait_send()
    own_to_partner.wait_send()
    for d in range(1, Z):
        source = (z + Z - d) % Z
        pltpu.make_async_remote_copy(
            stats.at[source], stats.at[source], sz_sem.at[d - 1], rz_sem.at[d - 1],
            device_id={"sp": source}, device_id_type=MESH,
        ).wait_recv()
    everything = stats[...]
    tops, totals, sums = everything[:, 0], everything[:, 1], everything[:, 2]
    factor = jnp.exp(tops - jnp.max(tops, axis=0, keepdims=True))
    ro_ref[...] = (jnp.sum(sums * factor, axis=0) / jnp.sum(totals * factor, axis=0)).astype(ro_ref.dtype)
    for d in range(1, Z):
        z_copy(d).wait_send()
    for copy in outs:
        copy.wait()


def body(
    tokens, norm_gain, key_weight, value_weight, cum_gates, new_query, new_key, new_value, new_gate
):
    S, L, D = tokens.shape
    C = key_weight.shape[1]
    H = C // HD
    T = lax.axis_size("tp")
    Z = lax.axis_size("sp")
    X = T // CORES
    BL = T * L
    R = 16 if L % 16 == 0 else L
    NC = S * (L // R)
    bf, f32 = jnp.bfloat16, jnp.float32
    hbm = pl.BlockSpec(memory_space=pltpu.HBM)
    dma = pltpu.SemaphoreType.DMA
    far = max(X - 1, 1)
    return pl.pallas_call(
        functools.partial(kernel, (S, L, R, T, Z)),
        out_shape=(
            jax.ShapeDtypeStruct((S, BL, C), bf),
            jax.ShapeDtypeStruct((S, BL, C), bf),
            jax.ShapeDtypeStruct((S, C), bf),
        ),
        in_specs=[hbm] * 9,
        out_specs=(hbm, hbm, pl.BlockSpec(memory_space=pltpu.VMEM)),
        scratch_shapes=[
            pltpu.VMEM((T, S * L, D), bf),
            pltpu.VMEM((max(S * L, 2 * far * R), D), bf),
            pltpu.VMEM((D, 2 * C), bf),
            pltpu.VMEM((S, BL, C), bf),
            pltpu.VMEM((S, BL, C), bf),
            pltpu.VMEM((1, D), bf),
            pltpu.VMEM((S, H, BL), f32),
            pltpu.VMEM((S, C), bf),
            pltpu.VMEM((S, C), bf),
            pltpu.VMEM((S, C), bf),
            pltpu.VMEM((S, H), f32),
            pltpu.VMEM((Z, 3, S, C), f32),
            dma((NC,)), dma((2,)), dma((6,)), dma((2,)),
            dma((far, NC)), dma((far, NC)), dma, dma,
            dma((far, NC)), dma((far, NC)), dma((max(Z - 1, 1),)), dma((max(Z - 1, 1),)),
        ],
        compiler_params=pltpu.CompilerParams(
            collective_id=0, has_side_effects=True, vmem_limit_bytes=56 * 1024 * 1024
        ),
    )(
        tokens.reshape(S * L, D),
        norm_gain.reshape(1, D),
        key_weight,
        value_weight,
        jnp.transpose(cum_gates, (0, 2, 1)),
        new_query,
        new_key,
        new_value,
        new_gate,
    )


def solution(mesh):
    in_specs = (
        P("gr", ("sp", "tp"), None),
        P(),
        P(None, "tp"),
        P(None, "tp"),
        P("gr", "sp", "tp"),
        P("gr", "tp"),
        P("gr", "tp"),
        P("gr", "tp"),
        P("gr", "tp"),
    )
    out_specs = (P("gr", "sp", "tp"), P("gr", "sp", "tp"), P("gr", "tp"))
    return jax.shard_map(body, mesh=mesh, in_specs=in_specs, out_specs=out_specs, check_vma=False)
```

```python
import functools

import jax
import jax.numpy as jnp
from jax import lax
from jax.experimental import pallas as pl
from jax.experimental.pallas import tpu as pltpu
from jax.sharding import PartitionSpec as P

HD = 64
CORES = 2

epsilon = 1e-06
masked_score = -1e30
MESH = pl.DeviceIdType.MESH


def kernel(
    dims,
    tok_hbm, gain_hbm, wk_hbm, wv_hbm, gates_hbm, q_hbm, nk_hbm, nv_hbm, ng_hbm,
    kbuf, vbuf, ro_ref,
    tok, inv, nb, acc, wbuf, gain_v, gain_row, gates_v, q_v, nk_v, nv_v, ng_v, stats,
    loc_sem, w_sem, small_sem, hop_sem,
    sx_sem, rx_sem, sp_sem, rp_sem, sr_sem, rr_sem, sz_sem, rz_sem,
):
    S, L, R, T, Z = dims
    X = T // CORES
    rows_each, D = tok.shape
    NC, KC = nb.shape[1], nb.shape[3]
    blocks = rows_each // R
    C = kbuf.shape[2]
    H = C // HD
    BL = T * L
    tp = lax.axis_index("tp")
    z = lax.axis_index("sp")
    x, c = tp // CORES, tp % CORES
    partner = x * CORES + (CORES - 1 - c)

    def rows(j):
        return pl.ds(j * R, R)

    loads = [pltpu.make_async_copy(tok_hbm.at[rows(j)], tok.at[rows(j)], loc_sem.at[j]) for j in range(blocks)]
    for copy in loads:
        copy.start()
    w_copies = [
        pltpu.make_async_copy(wk_hbm, wbuf.at[:, pl.ds(0, C)], w_sem.at[0]),
        pltpu.make_async_copy(wv_hbm, wbuf.at[:, pl.ds(C, C)], w_sem.at[1]),
    ]
    small = [
        pltpu.make_async_copy(src, dst, small_sem.at[i])
        for i, (src, dst) in enumerate(
            [(gain_hbm, gain_v), (gates_hbm, gates_v), (q_hbm, q_v), (nk_hbm, nk_v), (nv_hbm, nv_v), (ng_hbm, ng_v)]
        )
    ]
    for copy in small:
        copy.start()
    barrier = pltpu.get_barrier_semaphore()
    pl.semaphore_signal(barrier, inc=1, device_id={"tp": partner}, device_id_type=MESH)
    for d in range(1, X):
        pl.semaphore_signal(
            barrier, inc=1, device_id={"tp": ((x + d) % X) * CORES + c}, device_id_type=MESH
        )
    sides = (z > 0).astype(jnp.int32) + (z < Z - 1).astype(jnp.int32)

    def greet_sides(sem):
        @pl.when(z > 0)
        def _():
            pl.semaphore_signal(sem, inc=1, device_id={"sp": z - 1}, device_id_type=MESH)

        @pl.when(z < Z - 1)
        def _():
            pl.semaphore_signal(sem, inc=1, device_id={"sp": z + 1}, device_id_type=MESH)

    greet_sides(barrier)

    small[0].wait()
    g = gain_v[...].astype(jnp.float32)
    lanes = g.shape[1]
    for i in range(g.shape[0]):
        gain_row[:, pl.ds(i * lanes, lanes)] = g[i : i + 1, :]
    for j in range(blocks):
        loads[j].wait()
        if j == blocks - 1:
            for copy in w_copies:
                copy.start()
        v = tok[rows(j), :].astype(jnp.float32)
        r = lax.rsqrt(jnp.mean(v * v, axis=-1, keepdims=True) + epsilon)
        inv[rows(j), :] = jnp.broadcast_to(r, (R, KC))

    def x_copy(d, j):
        return pltpu.make_async_remote_copy(
            nb.at[tp, j], nb.at[tp, j], sx_sem.at[d - 1, j], rx_sem.at[d - 1, j],
            device_id={"tp": ((x + d) % X) * CORES + c}, device_id_type=MESH,
        )

    def x_source(d, core):
        return ((x + X - d) % X) * CORES + core

    def relay_copy(d, j):
        t = x_source(d, c)
        return pltpu.make_async_remote_copy(
            nb.at[t, j], nb.at[t, j], sr_sem.at[d - 1, j], rr_sem.at[d - 1, j],
            device_id={"tp": partner}, device_id_type=MESH,
        )

    def arrival(t, j, sem):
        return pltpu.make_async_remote_copy(
            nb.at[t, j], nb.at[t, j], sem, sem,
            device_id={"tp": partner}, device_id_type=MESH,
        )

    def norm(k):
        part = pl.ds(k * KC, KC)
        v = tok[:, part].astype(jnp.float32)
        nb[tp, k] = (v * inv[...] * gain_row[:, part]).astype(jnp.bfloat16)

    norm(0)
    norm(1)
    pl.semaphore_wait(barrier, 1 + (X - 1) + sides)
    for k in range(NC):
        for d in range(1, X):
            x_copy(d, k).start()
        if k + 2 < NC:
            norm(k + 2)
    own_to_partner = pltpu.make_async_remote_copy(
        nb.at[tp], nb.at[tp], sp_sem, rp_sem, device_id={"tp": partner}, device_id_type=MESH
    )
    own_to_partner.start()
    if Z > 2:
        greet_sides(hop_sem.at[0])

    for copy in small[1:]:
        copy.wait()
    acc[...] = jnp.zeros_like(acc)

    def project(group, k, first, second):
        part = pl.ds(pl.multiple_of(k * KC, KC), KC)
        both = jnp.concatenate([nb[first, k], nb[second, k]], axis=0)
        acc[group] += jnp.dot(both, wbuf[part, :], preferred_element_type=jnp.float32)

    def keep(group, first, second):
        for i, t in enumerate((first, second)):
            for s in range(S):
                y = acc[group, pl.ds(i * rows_each + s * L, L), :].astype(jnp.bfloat16)
                at = pl.ds(pl.multiple_of(t * L, L), L)
                kbuf[s, at, :] = y[:, :C]
                vbuf[s, at, :] = y[:, C:]

    for copy in w_copies:
        copy.wait()
    pltpu.make_async_remote_copy(
        nb.at[partner], nb.at[partner], sp_sem, rp_sem, device_id={"tp": partner}, device_id_type=MESH
    ).wait_recv()

    def near(k, carry):
        project(0, k, tp, partner)
        return carry

    lax.fori_loop(0, NC, near, 0)
    keep(0, tp, partner)
    for r in range(1, Z - 2):
        pl.semaphore_wait(hop_sem.at[r - 1], sides)
        greet_sides(hop_sem.at[r])

    def arrive(k):
        for d in range(1, X):
            arrival(x_source(d, c), k, rx_sem.at[d - 1, k]).wait_recv()
            relay_copy(d, k).start()

    def use(k):
        for d in range(1, X):
            first, second = x_source(d, c), x_source(d, CORES - 1 - c)
            arrival(second, k, rr_sem.at[d - 1, k]).wait_recv()
            project(d, k, first, second)

    def far(k, carry):
        arrive(k)
        use(k - 1)
        return carry

    arrive(0)
    lax.fori_loop(1, NC, far, 0)
    use(NC - 1)
    for d in range(1, X):
        keep(d, x_source(d, c), x_source(d, CORES - 1 - c))

    scale = HD ** (-0.5)
    head_of_lane = lax.broadcasted_iota(jnp.int32, (H, C), 1) // HD
    own_head = head_of_lane == lax.broadcasted_iota(jnp.int32, (H, C), 0)
    eye = lax.broadcasted_iota(jnp.int32, (H, H), 0) == lax.broadcasted_iota(jnp.int32, (H, H), 1)
    last_block = z == Z - 1

    def as_row(column):
        return jnp.sum(jnp.where(own_head, column, 0.0), axis=0, keepdims=True)

    for s in range(S):
        qd = jnp.where(own_head, q_v[s : s + 1, :].astype(jnp.float32), 0.0)
        fresh = jnp.sum(qd * nk_v[s : s + 1, :].astype(jnp.float32), axis=1, keepdims=True) * scale
        gates = gates_v[s]
        own_gate = jnp.sum(jnp.where(eye, ng_v[s : s + 1, :], 0.0), axis=1, keepdims=True)
        fresh = jnp.where(last_block, fresh - (gates[:, BL - 1 : BL] + own_gate), masked_score)
        scores = lax.dot_general(
            qd.astype(jnp.bfloat16), kbuf[s], (((1,), (1,)), ((), ())), preferred_element_type=jnp.float32
        )
        scores = scores * scale - gates
        top = jnp.maximum(jnp.max(scores, axis=1, keepdims=True), fresh)
        weights = jnp.exp(scores - top)
        fresh_weight = jnp.exp(fresh - top)
        total = jnp.sum(weights, axis=1, keepdims=True) + fresh_weight
        high = weights.astype(jnp.bfloat16)
        low = (weights - high.astype(jnp.float32)).astype(jnp.bfloat16)
        values = vbuf[s]
        weighted = jnp.dot(high, values, preferred_element_type=jnp.float32)
        weighted = weighted + jnp.dot(low, values, preferred_element_type=jnp.float32)
        weighted = weighted + fresh_weight * nv_v[s : s + 1, :].astype(jnp.float32)
        stats[z, 0, s : s + 1, :] = as_row(top)
        stats[z, 1, s : s + 1, :] = as_row(total)
        stats[z, 2, s : s + 1, :] = as_row(weighted)

    def z_copy(d):
        return pltpu.make_async_remote_copy(
            stats.at[z], stats.at[z], sz_sem.at[d - 1], rz_sem.at[d - 1],
            device_id={"sp": (z + d) % Z}, device_id_type=MESH,
        )

    if Z > 2:
        pl.semaphore_wait(hop_sem.at[Z - 3], sides)
    for d in range(1, Z):
        z_copy(d).start()
    for d in range(1, X):
        for j in range(NC):
            x_copy(d, j).wait_send()
            relay_copy(d, j).wait_send()
    own_to_partner.wait_send()
    for d in range(1, Z):
        source = (z + Z - d) % Z
        pltpu.make_async_remote_copy(
            stats.at[source], stats.at[source], sz_sem.at[d - 1], rz_sem.at[d - 1],
            device_id={"sp": source}, device_id_type=MESH,
        ).wait_recv()
    everything = stats[...]
    tops, totals, sums = everything[:, 0], everything[:, 1], everything[:, 2]
    factor = jnp.exp(tops - jnp.max(tops, axis=0, keepdims=True))
    ro_ref[...] = (jnp.sum(sums * factor, axis=0) / jnp.sum(totals * factor, axis=0)).astype(ro_ref.dtype)
    for d in range(1, Z):
        z_copy(d).wait_send()


def write_out(*refs):
    sems = refs[-1]
    count = (len(refs) - 1) // 2
    copies = [pltpu.make_async_copy(refs[i], refs[count + i], sems.at[i]) for i in range(count)]
    for copy in copies:
        copy.start()
    for copy in copies:
        copy.wait()


def body(
    tokens, norm_gain, key_weight, value_weight, cum_gates, new_query, new_key, new_value, new_gate
):
    S, L, D = tokens.shape
    C = key_weight.shape[1]
    H = C // HD
    T = lax.axis_size("tp")
    Z = lax.axis_size("sp")
    X = T // CORES
    BL = T * L
    R = 16 if L % 16 == 0 else L
    KC = 256 if D % 256 == 0 else D // 2
    NC = D // KC
    bf, f32 = jnp.bfloat16, jnp.float32
    hbm = pl.BlockSpec(memory_space=pltpu.HBM)
    dma = pltpu.SemaphoreType.DMA
    far = max(X - 1, 1)
    vmem = pl.BlockSpec(memory_space=pltpu.VMEM)
    results = pl.pallas_call(
        functools.partial(kernel, (S, L, R, T, Z)),
        out_shape=(
            pltpu.VMEM((S, BL, C), bf),
            pltpu.VMEM((S, BL, C), bf),
            pltpu.VMEM((S, C), bf),
        ),
        in_specs=[hbm] * 9,
        out_specs=(vmem, vmem, vmem),
        scratch_shapes=[
            pltpu.VMEM((S * L, D), bf),
            pltpu.VMEM((S * L, KC), f32),
            pltpu.VMEM((T, NC, S * L, KC), bf),
            pltpu.VMEM((X, 2 * S * L, 2 * C), f32),
            pltpu.VMEM((D, 2 * C), bf),
            pltpu.VMEM((D // 128, 128), bf),
            pltpu.VMEM((1, D), f32),
            pltpu.VMEM((S, H, BL), f32),
            pltpu.VMEM((S, C), bf),
            pltpu.VMEM((S, C), bf),
            pltpu.VMEM((S, C), bf),
            pltpu.VMEM((S, H), f32),
            pltpu.VMEM((Z, 3, S, C), f32),
            dma((S * L // R,)), dma((2,)), dma((6,)), pltpu.SemaphoreType.REGULAR((max(Z - 2, 1),)),
            dma((far, NC)), dma((far, NC)), dma, dma,
            dma((far, NC)), dma((far, NC)), dma((max(Z - 1, 1),)), dma((max(Z - 1, 1),)),
        ],
        compiler_params=pltpu.CompilerParams(
            collective_id=0, has_side_effects=True, vmem_limit_bytes=56 * 1024 * 1024
        ),
    )(
        tokens.reshape(S * L, D),
        norm_gain.reshape(D // 128, 128),
        key_weight,
        value_weight,
        jnp.transpose(cum_gates, (0, 2, 1)),
        new_query,
        new_key,
        new_value,
        new_gate,
    )
    return pl.pallas_call(
        write_out,
        out_shape=tuple(jax.ShapeDtypeStruct(r.shape, r.dtype) for r in results),
        in_specs=[vmem] * 3,
        out_specs=(hbm, hbm, hbm),
        scratch_shapes=[dma((3,))],
    )(*(pltpu.with_memory_space_constraint(r, pltpu.VMEM) for r in results))


def solution(mesh):
    in_specs = (
        P("gr", ("sp", "tp"), None),
        P(),
        P(None, "tp"),
        P(None, "tp"),
        P("gr", "sp", "tp"),
        P("gr", "tp"),
        P("gr", "tp"),
        P("gr", "tp"),
        P("gr", "tp"),
    )
    out_specs = (P("gr", "sp", "tp"), P("gr", "sp", "tp"), P("gr", "tp"))
    return jax.shard_map(body, mesh=mesh, in_specs=in_specs, out_specs=out_specs, check_vma=False)
```
